256 devices in a mesh: ep: 32 (over z, x), tp: 8 (over y, core).
Axes of the slice: x: 4, y: 4, z: 8, core: 2. Of those that a mesh axis runs over, the one named last changes fastest.
Arguments:
- tokens: bfloat16 [2048, 4096], P('ep'), may hold values from -6 to 6
- state_in: float32 [2048, 4096], P('ep', 'tp'), may hold values from -6 to 6
- conv_in: bfloat16 [2048, 3, 4096], P('ep', None, 'tp'), may hold values from -6 to 6
- mix_gain: bfloat16 [4096], replicated, may hold values from 0.099609375 to 1.8984375
- rnn_weight: bfloat16 [4096, 4096], P('ep', 'tp'), may hold values from -0.09375 to 0.09375
- gate_weight: bfloat16 [4096, 4096], P('ep', 'tp'), may hold values from -0.09375 to 0.09375
- conv_weight: bfloat16 [4, 4096], P(None, 'tp'), may hold values from -3 to 3
- rate_weight: bfloat16 [16, 256, 256], P('tp'), may hold values from -0.375 to 0.375
- input_weight: bfloat16 [16, 256, 256], P('tp'), may hold values from -0.375 to 0.375
- rate_param: float32 [4096], P('tp'), may hold values from 1 to 6
- out_weight: bfloat16 [4096, 4096], P('tp'), may hold values from -0.09375 to 0.09375
- moe_gain: bfloat16 [4096], replicated, may hold values from 0.099609375 to 1.8984375
- expert_gate: bfloat16 [32, 4096, 2048], P('ep', None, 'tp'), may hold values from -0.09375 to 0.09375
- expert_up: bfloat16 [32, 4096, 2048], P('ep', None, 'tp'), may hold values from -0.09375 to 0.09375
- expert_down: bfloat16 [32, 2048, 4096], P('ep', 'tp'), may hold values from -0.125 to 0.125
- routes: int32 [2048, 2], P('ep'), may hold values from 0 to 31, all different within a row; in each aligned block of 64 rows (0 to 63, 64 to 127, ...) at most 8 rows name the same one
- route_prob: float32 [2048, 2], P('ep'), may hold values from 0.1 to 1
Outputs:
- layer_out: bfloat16 [2048, 4096], P('ep', 'tp')
- state_out: float32 [2048, 4096], P('ep', 'tp')
- conv_out: bfloat16 [2048, 3, 4096], P('ep', None, 'tp')
The draws below stay inside these ranges and needn't reach their ends.
Inputs may be any that keep to these rules, and one draw needn't show every extreme that they name: `routes`: the 2 experts of a sequence differ. Among the rows of one index of ep no expert is named more than 8 times, and in every draw some expert is named exactly 8 times there.
All inputs are finite; a program needn't handle non-finite values.
Results may differ from the reference program's by a relative error of at most 0.014.
Values may be sent and summed in bfloat16 or wider, within the bound.
A program may use at most 64 MiB of HBM per device.

```python
import math
import jax
import jax.numpy as jnp
import numpy as np
from jax import lax

D = 4096
D_RNN = 4096
RG_BLOCKS = 16
RG_BW = 256
FF_E = 2048
TOPK = 2
SEQ_GRP = 64
BATCH = 2048
EXPERTS = 32
CAP = 8
N_EP = 32
N_TP = 8


def shard_levels(rng, extent, split, low, high):
    def one(dim, shards_of):
        steps = jax.random.uniform(jax.random.fold_in(jax.random.fold_in(rng, 6), dim), (shards_of,), jnp.float32, low / len(split), high / len(split))
        return jnp.repeat(jnp.exp(steps), extent[dim] // shards_of).reshape((-1,) + (1,) * (len(extent) - dim - 1))

    loudness = one(*split[0])
    for cut in split[1:]:
        loudness = loudness * one(*cut)
    return loudness


def assign_block(key, own, number, rows, amount, top, reach, lean):
    ranking = jax.random.permutation(key, amount)
    crowded, ordinary = portions_of(amount, rows * top, reach, lean, True), portions_of(amount, rows * top, reach, lean, False)
    places = jnp.arange(amount)

    def named(tallies, offset_by):
        used = int((tallies > 0).sum())
        fixed = max(1, used // 4)
        passed = fixed + (places - fixed + offset_by * (used - fixed)) % max(1, amount - fixed)
        return jnp.zeros((amount,), jnp.int32).at[ranking[jnp.where(places < fixed, places, passed)]].set(jnp.asarray(tallies, jnp.int32))

    tallies = jnp.where(number % 4 == 0, named(crowded, number // 4), named(ordinary, number - number // 4 - 1))
    mixed = jax.random.permutation(jax.random.fold_in(own, 3), amount)
    source_of, taker = mixed[0:amount // 2 * 2:2], mixed[1:amount // 2 * 2:2]
    room = jnp.minimum(tallies[source_of] - 1, reach - tallies[taker]) // 2
    room = jnp.where((source_of == ranking[0]) | (taker == ranking[0]) | (tallies[taker] == 0), 0, jnp.maximum(room, 0))
    passed = jax.random.randint(jax.random.fold_in(own, 4), (amount // 2,), 0, 1 << 20) % (room + 1)
    tallies = tallies.at[source_of].add(-passed).at[taker].add(passed)
    items = jnp.searchsorted(jnp.cumsum(tallies), jnp.arange(rows * top), side="right").astype(jnp.int32)
    table = items.reshape(top, rows).T
    table = table[jax.random.permutation(jax.random.fold_in(own, 1), rows)]
    offset_by = jax.random.randint(jax.random.fold_in(own, 2), (rows, 1), 0, top)
    return jnp.take_along_axis(table, (jnp.arange(top)[None, :] + offset_by) % top, axis=1)


def portions_of(number_of, total, limit, slope, full):
    portions = [(1 << 20) // math.isqrt(standing ** slope) + 1 for standing in range(1, number_of + 1)]
    largest = limit if full else min(limit, max(-(-total // number_of), total * portions[0] // sum(portions)))
    least = 1 if total - largest >= number_of - 1 else 0
    given, spare = [largest] + [least] * (number_of - 1), total - largest - least * (number_of - 1)
    while spare > 0:
        movable = [i for i in range(1, number_of) if given[i] < largest] or [i for i in range(1, number_of) if given[i] < limit]
        whole, budget = sum([portions[i] for i in movable]), spare
        for i in movable:
            addition = min(limit - given[i], max(1, budget * portions[i] // whole), spare)
            given[i] = given[i] + addition
            spare = spare - addition
    return np.array(given)


def scatter_about(own_key, dims, scale, limit, shards=(), held_as=jnp.bfloat16):
    level = shard_levels(own_key, dims, shards, -0.22, 0.18) if shards else 1.0
    drawn = jax.random.normal(own_key, dims, jnp.float32) * scale * level
    return jnp.minimum(jnp.maximum(drawn, -limit), limit).astype(held_as)


def setup_inputs(seed: int = 0) -> dict:
    streams_of = jax.random.split(jax.random.key(seed), 18)
    tokens = scatter_about(streams_of[0], (BATCH, D), 1.0, 6.0, ((0, 32),))
    state_in = scatter_about(streams_of[1], (BATCH, D_RNN), 1.0, 6.0, ((0, 32), (1, 8)), jnp.float32)
    conv_in = scatter_about(streams_of[2], (BATCH, 3, D_RNN), 1.0, 6.0, ((0, 32), (2, 8)))
    mix_gain = jnp.clip(1.0 + 0.18 * jax.random.normal(streams_of[3], (D,), jnp.float32), 0.099609375, 1.8984375).astype(jnp.bfloat16)
    rnn_weight = scatter_about(streams_of[4], (D, D_RNN), D ** -0.5, 0.09375, ((0, 32), (1, 8)))
    gate_weight = scatter_about(streams_of[5], (D, D_RNN), D ** -0.5, 0.09375, ((0, 32), (1, 8)))
    conv_weight = scatter_about(streams_of[6], (4, D_RNN), 0.5, 3.0, ((1, 8),))
    rate_weight = scatter_about(streams_of[7], (RG_BLOCKS, RG_BW, RG_BW), RG_BW ** -0.5, 0.375, ((0, 8),))
    input_weight = scatter_about(streams_of[8], (RG_BLOCKS, RG_BW, RG_BW), RG_BW ** -0.5, 0.375, ((0, 8),))
    rate_param = jnp.clip(1.0 + 5.0 * jax.random.uniform(streams_of[9], (D_RNN,), jnp.float32) ** shard_levels(streams_of[9], (D_RNN,), ((0, 8),), -0.2, 0.2), 1.0, 6.0)
    out_weight = scatter_about(streams_of[10], (D_RNN, D), D_RNN ** -0.5, 0.09375, ((0, 8),))
    moe_gain = jnp.clip(1.0 + 0.18 * jax.random.normal(streams_of[11], (D,), jnp.float32), 0.099609375, 1.8984375).astype(jnp.bfloat16)
    expert_gate = scatter_about(streams_of[12], (EXPERTS, D, FF_E), D ** -0.5, 0.09375, ((0, 32), (2, 8)))
    expert_up = scatter_about(streams_of[13], (EXPERTS, D, FF_E), D ** -0.5, 0.09375, ((0, 32), (2, 8)))
    expert_down = scatter_about(streams_of[14], (EXPERTS, FF_E, D), FF_E ** -0.5, 0.125, ((0, 32), (1, 8)))
    routes_keys = jax.random.split(jax.random.fold_in(streams_of[15], 1), BATCH // SEQ_GRP)
    routes_turns = jax.random.permutation(jax.random.fold_in(streams_of[15], 3), BATCH // SEQ_GRP)
    routes = jax.vmap(lambda own, number: assign_block(jax.random.fold_in(streams_of[15], 2), own, number, SEQ_GRP, EXPERTS, TOPK, CAP, 2))(routes_keys, routes_turns).reshape((BATCH, TOPK))
    route_prob = jnp.clip(0.1 + 0.9 * jax.random.uniform(streams_of[16], (BATCH, TOPK), jnp.float32) ** shard_levels(streams_of[16], (BATCH, TOPK), ((0, 32),), -0.2, 0.2), 0.1, 1.0)
    return dict(tokens=tokens, state_in=state_in, conv_in=conv_in, mix_gain=mix_gain, rnn_weight=rnn_weight, gate_weight=gate_weight, conv_weight=conv_weight, rate_weight=rate_weight, input_weight=input_weight, rate_param=rate_param, out_weight=out_weight, moe_gain=moe_gain, expert_gate=expert_gate, expert_up=expert_up, expert_down=expert_down, routes=routes, route_prob=route_prob)


def rms_scale(values, gain):
    scale = lax.rsqrt(lax.optimization_barrier(jnp.mean(values * values, axis=-1, keepdims=True)) + 1e-06)
    return values * scale * gain.astype(jnp.float32)

def slot_targets(route_ids, experts, capacity):
    flat_ids = route_ids.reshape(-1)
    onehot = (flat_ids[:, None] == jnp.arange(experts, dtype=jnp.int32)[None, :]).astype(jnp.int32)
    before = jnp.cumsum(onehot, axis=0) - onehot
    slot_ids = lax.optimization_barrier(jnp.sum(before * onehot, axis=1))
    return (flat_ids * capacity + slot_ids).astype(jnp.int32)

def block_map(conv, weight):
    rows = conv.shape[0]
    parts = conv.reshape(rows, RG_BLOCKS, RG_BW).astype(jnp.float32)
    mapped = jnp.einsum('snc,ncd->snd', parts, weight.astype(jnp.float32))
    return mapped.reshape(rows, D_RNN)

def run_expert(args):
    rows, w_gate, w_up, w_down = args
    rows32 = rows.astype(jnp.float32)
    gate_part = jnp.dot(rows32, w_gate.astype(jnp.float32))
    up_part = jnp.dot(rows32, w_up.astype(jnp.float32))
    hidden = (jax.nn.silu(gate_part) * up_part).astype(jnp.bfloat16)
    split_hidden = hidden.reshape(rows.shape[0], N_TP, FF_E // N_TP).astype(jnp.float32)
    split_down = w_down.reshape(N_TP, FF_E // N_TP, D).astype(jnp.float32)
    pieces = jnp.einsum('rtf,tfd->trd', split_hidden, split_down)
    rounded = lax.optimization_barrier(pieces.astype(jnp.bfloat16)).astype(jnp.float32)
    return lax.optimization_barrier(jnp.sum(rounded, axis=0)).astype(jnp.bfloat16)

def reference(tokens, state_in, conv_in, mix_gain, rnn_weight, gate_weight, conv_weight, rate_weight, input_weight, rate_param, out_weight, moe_gain, expert_gate, expert_up, expert_down, routes, route_prob):
    base = tokens.astype(jnp.float32)
    normed = rms_scale(base, mix_gain).astype(jnp.bfloat16)
    proj_x = jnp.dot(normed, rnn_weight, preferred_element_type=jnp.float32)
    proj_y = jnp.dot(normed, gate_weight, preferred_element_type=jnp.float32)
    moved = proj_x.astype(jnp.bfloat16)
    conv_out = jnp.concatenate([conv_in[:, 1:], moved[:, None, :]], axis=1)
    taps = conv_weight.astype(jnp.float32)
    history = conv_in.astype(jnp.float32)
    summed = history[:, 0] * taps[0] + history[:, 1] * taps[1] + history[:, 2] * taps[2] + moved.astype(jnp.float32) * taps[3]
    conv = summed.astype(jnp.bfloat16)
    rate = jax.nn.sigmoid(block_map(conv, rate_weight))
    in_gate = jax.nn.sigmoid(block_map(conv, input_weight))
    log_decay = -8.0 * rate * jax.nn.softplus(-rate_param)
    state_out = jnp.exp(log_decay) * state_in + jnp.sqrt(-jnp.expm1(2.0 * log_decay)) * in_gate * conv.astype(jnp.float32)
    gated = (state_out * jax.nn.gelu(proj_y, approximate=True)).astype(jnp.bfloat16)
    split_gated = gated.reshape(BATCH, N_TP, D_RNN // N_TP).astype(jnp.float32)
    split_out = out_weight.reshape(N_TP, D_RNN // N_TP, D).astype(jnp.float32)
    pieces = jnp.einsum('btc,tcd->tbd', split_gated, split_out)
    rounded = lax.optimization_barrier(pieces.astype(jnp.bfloat16)).astype(jnp.float32)
    mixed = base + lax.optimization_barrier(jnp.sum(rounded, axis=0))
    normed2 = rms_scale(mixed, moe_gain).astype(jnp.bfloat16)
    group_routes = routes.reshape(N_EP, SEQ_GRP * TOPK)
    targets = jax.vmap(lambda group_ids: slot_targets(group_ids, EXPERTS, CAP))(group_routes)
    dispatch = (jnp.arange(EXPERTS * CAP, dtype=jnp.int32)[None, :, None] == targets[:, None, :]).astype(jnp.float32)
    repeated = jnp.repeat(normed2, TOPK, axis=0).reshape(N_EP, SEQ_GRP * TOPK, D).astype(jnp.float32)
    send = jnp.einsum('grj,gjd->grd', dispatch, repeated).astype(jnp.bfloat16)
    by_expert = send.reshape(N_EP, EXPERTS, CAP, D).transpose(1, 0, 2, 3).reshape(EXPERTS, N_EP * CAP, D)
    outputs = lax.map(run_expert, (by_expert, expert_gate, expert_up, expert_down))
    back = outputs.reshape(EXPERTS, N_EP, CAP, D).transpose(1, 0, 2, 3).reshape(N_EP, EXPERTS * CAP, D).astype(jnp.float32)
    picked = jnp.einsum('grj,grd->gjd', dispatch, back).reshape(BATCH, TOPK, D)
    weights = route_prob / lax.optimization_barrier(jnp.sum(route_prob, axis=1, keepdims=True))
    experts_sum = lax.optimization_barrier(jnp.sum(picked * weights[:, :, None], axis=1))
    layer_out = (mixed + experts_sum).astype(jnp.bfloat16)
    return (layer_out, state_out, conv_out)
```

```python
import functools

import jax
import jax.numpy as jnp
from jax import lax
from jax.experimental import pallas as pl
from jax.experimental.pallas import tpu as pltpu
from jax.sharding import PartitionSpec as P

NX = 4
NY = 4
NC = 2
MESH = pl.DeviceIdType.MESH
F32 = jnp.float32
BF16 = jnp.bfloat16


def dot(a, b):
    return jnp.dot(a, b, preferred_element_type=F32)


def dot_t(a, b):
    return lax.dot_general(a, b, (((0,), (0,)), ((), ())), preferred_element_type=F32)


def layer_kernel(
    tokens,
    hist,
    state_in,
    mix_gain,
    rnn_w,
    gate_w,
    tap,
    rate_w,
    input_w,
    rate_param,
    moe_gain,
    routes,
    prob,
    out_w_hbm,
    eg_hbm,
    eu_hbm,
    ed_hbm,
    layer_out,
    state_out,
    moved_out,
    out_w,
    wgu,
    wd,
    nrm,
    acts,
    wbuf,
    pbuf,
    rs_send,
    rs_recv,
    os_send,
    os_recv,
    oy_send,
    oy_recv,
    sd,
    gbuf,
    xg,
    acc,
    d_send,
    d_recv,
    qf,
    q_send,
    fw_recv,
    fin_recv,
    back_send,
    back_recv,
    local_sem,
    w_ssem,
    w_rsem,
    a_ssem,
    a_rsem,
    ad_ssem,
    ad_rsem,
    rs_ssem,
    rs_rsem,
    os_ssem,
    os_rsem,
    oy_ssem,
    oy_rsem,
    s_ssem,
    s_rsem,
    ag_ssem,
    ag_rsem,
    d_ssem,
    d_rsem,
    q_ssem,
    fw_rsem,
    fin_rsem,
    b_ssem,
    b_rsem,
):
    rows, width = tokens.shape
    chan = rnn_w.shape[1]
    ks = rnn_w.shape[0]
    ep_n = width // ks
    nz = ep_n // NX
    half_z = nz // 2
    tp_n = NY * NC
    kz = width // nz
    kh = kz // 2
    ff = wd.shape[0]
    cap = sd.shape[0] // ep_n // 2
    ch = chan // 2
    slots = ep_n * cap

    ep = lax.axis_index("ep")
    tp = lax.axis_index("tp")
    z = ep // NX
    x = ep % NX
    y = tp // NC
    c = tp % NC
    other = (c + 1) % NC

    def epid(zz, xx):
        return (zz % nz) * NX + xx % NX

    def tpid(yy, cc):
        return (yy % NY) * NC + cc

    partner = tpid(y, other)
    started = []

    def send(src, dst, ssem, rsem, to_ep, to_tp):
        copy = pltpu.make_async_remote_copy(
            src_ref=src,
            dst_ref=dst,
            send_sem=ssem,
            recv_sem=rsem,
            device_id=(to_ep, to_tp),
            device_id_type=MESH,
        )
        copy.start()
        started.append(copy)

    def arrived(dst, ssem, rsem):
        pltpu.make_async_remote_copy(
            src_ref=dst,
            dst_ref=dst,
            send_sem=ssem,
            recv_sem=rsem,
            device_id=(ep, partner),
            device_id_type=MESH,
        ).wait_recv()

    load_ow = pltpu.make_async_copy(out_w_hbm, out_w, local_sem.at[0])
    load_eg = pltpu.make_async_copy(eg_hbm.at[0], wgu.at[:, pl.ds(0, ff)], local_sem.at[1])
    load_eu = pltpu.make_async_copy(eu_hbm.at[0], wgu.at[:, pl.ds(ff, ff)], local_sem.at[2])
    load_ed = pltpu.make_async_copy(ed_hbm.at[0], wd, local_sem.at[3])
    load_ow.start()
    load_eg.start()
    load_eu.start()
    load_ed.start()

    barrier = pltpu.get_barrier_semaphore()

    @pl.loop(1, ep_n)
    def _(i):
        pl.semaphore_signal(
            barrier, inc=1, device_id=((ep + i) % ep_n, tp), device_id_type=MESH
        )

    @pl.loop(1, tp_n)
    def _(i):
        pl.semaphore_signal(
            barrier, inc=1, device_id=(ep, (tp + i) % tp_n), device_id_type=MESH
        )

    base = tokens[...].astype(F32)
    scale = lax.rsqrt(jnp.mean(base * base, axis=-1, keepdims=True) + 1e-06)
    normed = (base * scale * mix_gain[...].astype(F32)).astype(BF16)
    for k in range(2 * nz):
        nrm[k] = normed[:, k * kh : (k + 1) * kh]
    wbuf[0, pl.ds(x * ks, ks), :] = rnn_w[...]
    wbuf[1, pl.ds(x * ks, ks), :] = gate_w[...]
    for h in range(2):
        acts[h, pl.ds(z * rows, rows), :] = nrm[2 * z + h]

    pl.semaphore_wait(barrier, ep_n - 1 + tp_n - 1)

    own_w = (rnn_w, gate_w)

    def w_slot(part, xx):
        return wbuf.at[part, pl.ds((xx % NX) * ks, ks), :]

    for n, (part, d) in enumerate(((0, 1), (1, -1), (1, 1), (0, -1))):
        send(
            own_w[part],
            w_slot(part, x),
            w_ssem.at[n],
            w_rsem.at[part, x],
            epid(z, x + d + NX),
            tp,
        )

    order = []
    for i in range(half_z, 0, -1):
        order.append(i)
        if i < half_z:
            order.append(nz - i)
    for i in order:
        to_z = (z + i) % nz
        send(
            nrm.at[2 * to_z + c],
            acts.at[c, pl.ds(z * rows, rows), :],
            a_ssem.at[i],
            a_rsem.at[z],
            epid(to_z, x),
            tp,
        )
    for i in reversed(order):
        from_z = (z + nz - i) % nz
        block = acts.at[c, pl.ds(from_z * rows, rows), :]
        arrived(block, a_ssem.at[i], a_rsem.at[from_z])
        send(block, block, ad_ssem.at[i], ad_rsem.at[from_z], ep, partner)

    left = (x + NX - 1) % NX
    right = (x + 1) % NX
    far = (x + 2) % NX
    arrived(w_slot(0, left), w_ssem.at[0], w_rsem.at[0, left])
    send(w_slot(0, left), w_slot(0, left), w_ssem.at[4], w_rsem.at[0, left], epid(z, right), tp)
    arrived(w_slot(1, right), w_ssem.at[0], w_rsem.at[1, right])
    send(w_slot(1, right), w_slot(1, right), w_ssem.at[5], w_rsem.at[1, right], epid(z, left), tp)
    arrived(w_slot(1, left), w_ssem.at[0], w_rsem.at[1, left])
    arrived(w_slot(0, right), w_ssem.at[0], w_rsem.at[0, right])
    for i in reversed(order):
        from_z = (z + nz - i) % nz
        block = acts.at[other, pl.ds(from_z * rows, rows), :]
        arrived(block, ad_ssem.at[i], ad_rsem.at[from_z])
    arrived(w_slot(0, far), w_ssem.at[0], w_rsem.at[0, far])
    arrived(w_slot(1, far), w_ssem.at[0], w_rsem.at[1, far])

    for part in range(2):
        pbuf[part] = dot(acts[0], wbuf[part, 0:kh, :]) + dot(acts[1], wbuf[part, kh:kz, :])

    chains = ((1, 0, 0), (-1, 1, 0), (1, 1, 1), (-1, 0, 1))

    def part_rows(part, zz):
        return pbuf[part, pl.ds((zz % nz) * rows, rows), :]

    for s in range(half_z):
        for n in (0, 1, 2, 3) if s == 0 else (2, 3, 0, 1):
            d, part, first = chains[n]
            if s < first:
                continue
            value = part_rows(part, z + nz + d * (half_z - s))
            if s > first:
                arrived(rs_recv.at[n, s - 1], rs_ssem.at[n, s], rs_rsem.at[n, s - 1])
                value = value + rs_recv[n, s - 1].astype(F32)
            rs_send[n, s] = value.astype(BF16)
            send(
                rs_send.at[n, s],
                rs_recv.at[n, s],
                rs_ssem.at[n, s],
                rs_rsem.at[n, s],
                epid(z + d + nz, x),
                tp,
            )
    last = half_z - 1
    for n in range(4):
        arrived(rs_recv.at[n, last], rs_ssem.at[n, last], rs_rsem.at[n, last])
    proj_x = part_rows(0, z) + rs_recv[0, last].astype(F32) + rs_recv[3, last].astype(F32)
    proj_y = part_rows(1, z) + rs_recv[1, last].astype(F32) + rs_recv[2, last].astype(F32)

    moved = proj_x.astype(BF16)
    moved_out[...] = moved
    conv = (hist[...] + moved.astype(F32) * tap[...].astype(F32)).astype(BF16)
    blocks, bw = rate_w.shape[0], rate_w.shape[1]
    rate = jnp.concatenate(
        [dot(conv[:, b * bw : (b + 1) * bw], rate_w[b]) for b in range(blocks)], axis=1
    )
    in_gate = jnp.concatenate(
        [dot(conv[:, b * bw : (b + 1) * bw], input_w[b]) for b in range(blocks)], axis=1
    )
    rate = jax.nn.sigmoid(rate)
    in_gate = jax.nn.sigmoid(in_gate)
    param = rate_param[...]
    soft = jnp.maximum(-param, 0.0) + jnp.log1p(jnp.exp(-jnp.abs(param)))
    log_decay = -8.0 * rate * soft
    tanh_decay = jnp.tanh(log_decay)
    rest = -2.0 * tanh_decay / (1.0 - tanh_decay)
    state = jnp.exp(log_decay) * state_in[...] + jnp.sqrt(rest) * in_gate * conv.astype(F32)
    state_out[...] = state
    gelu = 0.5 * proj_y * (
        1.0 + jnp.tanh(0.7978845608028654 * (proj_y + 0.044715 * proj_y * proj_y * proj_y))
    )
    gated = (state * gelu).astype(BF16)

    load_ow.wait()

    def out_cols(yy, cc):
        return pl.ds(pl.multiple_of(tpid(yy, cc) * chan, chan), chan)

    for i in (2, 1, 3, 0):
        yy = (y + i) % NY
        os_send[i] = dot(gated, out_w[:, out_cols(yy, other)]).astype(BF16)
        send(os_send.at[i], os_recv.at[i], os_ssem.at[i], os_rsem.at[i], ep, partner)
    for i in (2, 1, 3):
        yy = (y + i) % NY
        value = dot(gated, out_w[:, out_cols(yy, c)])
        arrived(os_recv.at[i], os_ssem.at[i], os_rsem.at[i])
        oy_send[i] = (value + os_recv[i].astype(F32)).astype(BF16)
        send(oy_send.at[i], oy_recv.at[i], oy_ssem.at[i], oy_rsem.at[i], ep, tpid(yy, c))
    mixed = tokens[:, out_cols(y, c)].astype(F32) + dot(gated, out_w[:, out_cols(y, c)])

    lanes = lax.broadcasted_iota(jnp.int32, (rows, ep_n), 1)
    one0 = (routes[:, 0:1] == lanes).astype(F32)
    one1 = (routes[:, 1:2] == lanes).astype(F32)
    lower = (
        lax.broadcasted_iota(jnp.int32, (rows, rows), 0)
        > lax.broadcasted_iota(jnp.int32, (rows, rows), 1)
    ).astype(F32)
    before = dot(lower.astype(BF16), (one0 + one1).astype(BF16))
    ids = lax.broadcasted_iota(jnp.int32, (rows, 2 * slots), 1).astype(F32)

    def one_hot(k, one):
        slot = jnp.sum(before * one, axis=1, keepdims=True)
        first = routes[:, k : k + 1].astype(F32) * (2.0 * cap) + slot
        return (ids == first).astype(F32), (ids == first + cap).astype(F32)

    lo0, hi0 = one_hot(0, one0)
    lo1, hi1 = one_hot(1, one1)
    lo_all = (lo0 + lo1).astype(BF16)
    hi_all = (hi0 + hi1).astype(BF16)

    arrived(os_recv.at[0], os_ssem.at[0], os_rsem.at[0])
    mixed = mixed + os_recv[0].astype(F32)
    for i in (1, 3, 2):
        arrived(oy_recv.at[i], oy_ssem.at[i], oy_rsem.at[i])
        mixed = mixed + oy_recv[i].astype(F32)
    mixed16 = mixed.astype(BF16)

    sd[...] = (dot_t(lo_all, mixed16[:, 0:ch]) + dot_t(hi_all, mixed16[:, ch:chan])).astype(BF16)
    tile = 2 * cap

    def slot_rows(e):
        return pl.ds(pl.multiple_of(e * tile, tile), tile)

    def scatter(src, dst_of, ssem, rsem):
        @pl.loop(1, ep_n)
        def _(i):
            e = (ep + i) % ep_n
            pltpu.make_async_remote_copy(
                src_ref=src.at[slot_rows(e), :],
                dst_ref=dst_of(ep),
                send_sem=ssem.at[i],
                recv_sem=rsem.at[ep],
                device_id=(e, tp),
                device_id_type=MESH,
            ).start()

    def gathered(src, dst_of, ssem, rsem):
        @pl.loop(1, ep_n)
        def _(i):
            e = (ep + i) % ep_n
            copy = pltpu.make_async_remote_copy(
                src_ref=src.at[slot_rows(e), :],
                dst_ref=dst_of(e),
                send_sem=ssem.at[i],
                recv_sem=rsem.at[e],
                device_id=(e, tp),
                device_id_type=MESH,
            )
            copy.wait_send()
            copy.wait_recv()

    def own_slot(e):
        return gbuf.at[tp, slot_rows(e), :]

    scatter(sd, own_slot, s_ssem, s_rsem)
    gbuf[tp, slot_rows(ep), :] = sd[slot_rows(ep), :]
    load_eg.wait()
    load_eu.wait()
    load_ed.wait()
    gathered(sd, own_slot, s_ssem, s_rsem)

    hrows = slots

    def half(t, h):
        return gbuf.at[t, pl.ds(h * hrows, hrows), :]

    counter = [0]

    def share(t, h, to_tp):
        send(half(t, h), half(t, h), ag_ssem.at[counter[0]], ag_rsem.at[t, h], ep, to_tp)
        counter[0] += 1

    def shared(t, h):
        arrived(half(t, h), ag_ssem.at[0], ag_rsem.at[t, h])

    up_tp = tpid(y + 1, c)
    down_tp = tpid(y + 3, c)
    far_tp = tpid(y + 2, c)
    share(tp, 0, up_tp)
    share(tp, 1, down_tp)
    share(tp, 1, up_tp)
    share(tp, 0, down_tp)
    share(tp, 0, partner)
    share(tp, 1, partner)

    squares = jnp.zeros((slots, 1), F32)

    def absorb(t, squares, first):
        value = gbuf[t].astype(F32).reshape(ep_n, 2 * cap, ch)
        parts = (value[:, 0:cap, :], value[:, cap:, :])
        for k in range(2):
            piece = parts[k].reshape(slots, ch)
            squares = squares + jnp.sum(piece * piece, axis=1, keepdims=True)
            at = pl.multiple_of(t * chan + k * ch, ch)
            piece = (piece * moe_gain[:, pl.ds(at, ch)].astype(F32)).astype(BF16)
            product = dot(piece, wgu[pl.ds(at, ch), :])
            if first and k == 0:
                acc[...] = product
            else:
                acc[...] += product
        return squares

    squares = absorb(tp, squares, True)
    shared(partner, 0)
    shared(partner, 1)
    squares = absorb(partner, squares, False)
    shared(down_tp, 0)
    share(down_tp, 0, up_tp)
    share(down_tp, 0, partner)
    shared(up_tp, 1)
    share(up_tp, 1, down_tp)
    share(up_tp, 1, partner)
    shared(down_tp, 1)
    share(down_tp, 1, partner)
    shared(up_tp, 0)
    share(up_tp, 0, partner)
    squares = absorb(down_tp, squares, False)
    squares = absorb(up_tp, squares, False)
    shared(far_tp, 0)
    share(far_tp, 0, partner)
    shared(far_tp, 1)
    share(far_tp, 1, partner)
    for i in (3, 1):
        t = tpid(y + i, other)
        shared(t, 0)
        shared(t, 1)
        squares = absorb(t, squares, False)
    squares = absorb(far_tp, squares, False)
    t = tpid(y + 2, other)
    shared(t, 0)
    shared(t, 1)
    squares = absorb(t, squares, False)

    scale2 = lax.rsqrt(squares * (1.0 / width) + 1e-06)
    gate_part = acc[:, 0:ff] * scale2
    up_part = acc[:, ff:] * scale2
    hidden = (gate_part * jax.nn.sigmoid(gate_part) * up_part).astype(BF16)

    for i in (2, 1, 3, 0):
        d_send[i] = dot(hidden, wd[:, out_cols(y + i, other)]).astype(BF16)
        send(d_send.at[i], d_recv.at[i], d_ssem.at[i], d_rsem.at[i], ep, partner)

    hs = slots // 2

    def own_part(i):
        value = dot(hidden, wd[:, out_cols(y + i, c)])
        arrived(d_recv.at[i], d_ssem.at[i], d_rsem.at[i])
        return value + d_recv[i].astype(F32)

    value = own_part(2)
    q_send[0] = value[0:hs].astype(BF16)
    send(q_send.at[0], fw_recv.at[0], q_ssem.at[0], fw_rsem.at[0], ep, up_tp)
    q_send[1] = value[hs:].astype(BF16)
    send(q_send.at[1], fw_recv.at[1], q_ssem.at[1], fw_rsem.at[1], ep, down_tp)
    value = own_part(1)
    q_send[2] = value[hs:].astype(BF16)
    send(q_send.at[2], fin_recv.at[0, 1], q_ssem.at[2], fin_rsem.at[0, 1], ep, up_tp)
    qf[0] = value[0:hs]
    value = own_part(3)
    q_send[3] = value[0:hs].astype(BF16)
    send(q_send.at[3], fin_recv.at[1, 0], q_ssem.at[3], fin_rsem.at[1, 0], ep, down_tp)
    qf[1] = value[hs:]
    arrived(fw_recv.at[0], q_ssem.at[0], fw_rsem.at[0])
    q_send[4] = (qf[0] + fw_recv[0].astype(F32)).astype(BF16)
    send(q_send.at[4], fin_recv.at[0, 0], q_ssem.at[4], fin_rsem.at[0, 0], ep, up_tp)
    arrived(fw_recv.at[1], q_ssem.at[0], fw_rsem.at[1])
    q_send[5] = (qf[1] + fw_recv[1].astype(F32)).astype(BF16)
    send(q_send.at[5], fin_recv.at[1, 1], q_ssem.at[5], fin_rsem.at[1, 1], ep, down_tp)
    value = own_part(0)
    for h in range(2):
        total = value[h * hs : (h + 1) * hs]
        for d in range(2):
            arrived(fin_recv.at[d, h], q_ssem.at[0], fin_rsem.at[d, h])
            total = total + fin_recv[d, h].astype(F32)
        total = total.reshape(hs // cap, cap, chan)
        total = jnp.concatenate([total[:, :, 0:ch], total[:, :, ch:]], axis=1)
        back_send[h * slots : (h + 1) * slots, :] = total.reshape(slots, ch).astype(BF16)

    def back_slot(e):
        return back_recv.at[slot_rows(e), :]

    scatter(back_send, back_slot, b_ssem, b_rsem)
    back_recv[slot_rows(ep), :] = back_send[slot_rows(ep), :]
    p0 = prob[:, 0:1]
    p1 = prob[:, 1:2]
    inv = 1.0 / (p0 + p1)
    gathered(back_send, back_slot, b_ssem, b_rsem)
    returned = back_recv[...]
    w0 = p0 * inv
    w1 = p1 * inv
    for k, (a, b) in enumerate(((lo0, lo1), (hi0, hi1))):
        picked = w0 * dot(a.astype(BF16), returned) + w1 * dot(b.astype(BF16), returned)
        layer_out[:, k * ch : (k + 1) * ch] = (
            mixed[:, k * ch : (k + 1) * ch] + picked
        ).astype(BF16)

    for copy in started:
        copy.wait_send()


def shards(
    tokens,
    state_in,
    conv_in,
    mix_gain,
    rnn_weight,
    gate_weight,
    conv_weight,
    rate_weight,
    input_weight,
    rate_param,
    out_weight,
    moe_gain,
    expert_gate,
    expert_up,
    expert_down,
    routes,
    route_prob,
):
    rows, width = tokens.shape
    ks, chan = rnn_weight.shape
    ep_n = lax.axis_size("ep")
    tp_n = lax.axis_size("tp")
    nz = ep_n // NX
    half_z = nz // 2
    kh = width // nz // 2
    ff = expert_down.shape[1]
    topk = routes.shape[1]
    cap = max(2, 2 * rows * topk // ep_n)
    slots = ep_n * cap
    ch = chan // 2

    taps = conv_weight.astype(F32)
    history = conv_in.astype(F32)
    hist = history[:, 0] * taps[0] + history[:, 1] * taps[1] + history[:, 2] * taps[2]

    vm = pl.BlockSpec(memory_space=pltpu.VMEM)
    hbm = pl.BlockSpec(memory_space=pl.ANY)
    dma = pltpu.SemaphoreType.DMA
    layer_out, state_out, moved = pl.pallas_call(
        layer_kernel,
        out_shape=(
            jax.ShapeDtypeStruct((rows, chan), BF16),
            jax.ShapeDtypeStruct((rows, chan), F32),
            jax.ShapeDtypeStruct((rows, chan), BF16),
        ),
        in_specs=[vm] * 13 + [hbm] * 4,
        out_specs=(vm, vm, vm),
        scratch_shapes=[
            pltpu.VMEM((chan, width), BF16),
            pltpu.VMEM((width, 2 * ff), BF16),
            pltpu.VMEM((ff, width), BF16),
            pltpu.VMEM((2 * nz, rows, kh), BF16),
            pltpu.VMEM((2, nz * rows, kh), BF16),
            pltpu.VMEM((2, NX * ks, chan), BF16),
            pltpu.VMEM((2, nz * rows, chan), F32),
            pltpu.VMEM((4, half_z, rows, chan), BF16),
            pltpu.VMEM((4, half_z, rows, chan), BF16),
            pltpu.VMEM((NY, rows, chan), BF16),
            pltpu.VMEM((NY, rows, chan), BF16),
            pltpu.VMEM((NY, rows, chan), BF16),
            pltpu.VMEM((NY, rows, chan), BF16),
            pltpu.VMEM((2 * slots, ch), BF16),
            pltpu.VMEM((tp_n, 2 * slots, ch), BF16),
            pltpu.VMEM((16, 128), BF16),
            pltpu.VMEM((slots, 2 * ff), F32),
            pltpu.VMEM((NY, slots, chan), BF16),
            pltpu.VMEM((NY, slots, chan), BF16),
            pltpu.VMEM((2, slots // 2, chan), F32),
            pltpu.VMEM((6, slots // 2, chan), BF16),
            pltpu.VMEM((2, slots // 2, chan), BF16),
            pltpu.VMEM((2, 2, slots // 2, chan), BF16),
            pltpu.VMEM((2 * slots, ch), BF16),
            pltpu.VMEM((2 * slots, ch), BF16),
            dma((4,)),
            dma((6,)),
            dma((2, NX)),
            dma((nz,)),
            dma((nz,)),
            dma((nz,)),
            dma((nz,)),
            dma((4, half_z)),
            dma((4, half_z)),
            dma((NY,)),
            dma((NY,)),
            dma((NY,)),
            dma((NY,)),
            dma((ep_n,)),
            dma((ep_n,)),
            dma((14,)),
            dma((tp_n, 2)),
            dma((NY,)),
            dma((NY,)),
            dma((6,)),
            dma((2,)),
            dma((2, 2)),
            dma((ep_n,)),
            dma((ep_n,)),
        ],
        compiler_params=pltpu.CompilerParams(
            collective_id=0,
            has_side_effects=True,
            vmem_limit_bytes=60 * 1024 * 1024,
        ),
        name="layer",
    )(
        tokens,
        hist,
        state_in,
        mix_gain.reshape(1, width),
        rnn_weight,
        gate_weight,
        conv_weight[3:4],
        rate_weight,
        input_weight,
        rate_param.reshape(1, chan),
        moe_gain.reshape(1, width),
        routes,
        route_prob,
        out_weight,
        expert_gate,
        expert_up,
        expert_down,
    )
    conv_out = jnp.concatenate([conv_in[:, 1:], moved[:, None, :]], axis=1)
    return (layer_out, state_out, conv_out)


def solution(mesh):
    in_specs = (
        P("ep", None),
        P("ep", "tp"),
        P("ep", None, "tp"),
        P(),
        P("ep", "tp"),
        P("ep", "tp"),
        P(None, "tp"),
        P("tp", None, None),
        P("tp", None, None),
        P("tp"),
        P("tp", None),
        P(),
        P("ep", None, "tp"),
        P("ep", None, "tp"),
        P("ep", "tp", None),
        P("ep", None),
        P("ep", None),
    )
    out_specs = (P("ep", "tp"), P("ep", "tp"), P("ep", None, "tp"))
    return jax.shard_map(shards, mesh=mesh, in_specs=in_specs, out_specs=out_specs, check_vma=False)
```

```python
import functools

import jax
import jax.numpy as jnp
from jax import lax
from jax.experimental import pallas as pl
from jax.experimental.pallas import tpu as pltpu
from jax.sharding import PartitionSpec as P

NX = 4
NY = 4
NC = 2
MESH = pl.DeviceIdType.MESH
F32 = jnp.float32
BF16 = jnp.bfloat16


def dot(a, b):
    return jnp.dot(a, b, preferred_element_type=F32)


def dot_t(a, b):
    return lax.dot_general(a, b, (((0,), (0,)), ((), ())), preferred_element_type=F32)


class Phases:
    def __init__(self):
        self.scope = None

    def __call__(self, name):
        if self.scope is not None:
            self.scope.__exit__(None, None, None)
        self.scope = jax.named_scope(name) if name else None
        if self.scope is not None:
            self.scope.__enter__()


def layer_kernel(
    tokens,
    conv_in,
    state_in,
    mix_gain,
    rnn_w,
    gate_w,
    taps,
    rate_w,
    input_w,
    rate_param,
    moe_gain,
    routes,
    prob,
    out_w_hbm,
    eg_hbm,
    eu_hbm,
    ed_hbm,
    layer_out,
    state_out,
    conv_out,
    out_w,
    wgu,
    wd,
    nrm,
    acts,
    wbuf,
    pbuf,
    rs_send,
    rs_recv,
    os_send,
    os_recv,
    oy_send,
    oy_recv,
    sd,
    gbuf,
    gain2,
    acc,
    d_send,
    d_recv,
    qf,
    q_send,
    fw_recv,
    fin_recv,
    back_send,
    back_recv,
    local_sem,
    w_ssem,
    w_rsem,
    a_ssem,
    a_rsem,
    ad_ssem,
    ad_rsem,
    rs_ssem,
    rs_rsem,
    os_ssem,
    os_rsem,
    oy_ssem,
    oy_rsem,
    s_ssem,
    s_rsem,
    ag_ssem,
    ag_rsem,
    d_ssem,
    d_rsem,
    q_ssem,
    fw_rsem,
    fin_rsem,
    b_ssem,
    b_rsem,
):
    rows, width = tokens.shape
    chan = rnn_w.shape[1]
    ks = rnn_w.shape[0]
    ep_n = width // ks
    nz = ep_n // NX
    half_z = nz // 2
    tp_n = NY * NC
    kz = width // nz
    kh = kz // 2
    ff = wd.shape[0]
    cap = sd.shape[0] // ep_n // 2
    ch = chan // 2
    slots = ep_n * cap

    ep = lax.axis_index("ep")
    tp = lax.axis_index("tp")
    z = ep // NX
    x = ep % NX
    y = tp // NC
    c = tp % NC
    other = (c + 1) % NC

    def epid(zz, xx):
        return (zz % nz) * NX + xx % NX

    def tpid(yy, cc):
        return (yy % NY) * NC + cc

    partner = tpid(y, other)
    started = []

    def send(src, dst, ssem, rsem, to_ep, to_tp):
        copy = pltpu.make_async_remote_copy(
            src_ref=src,
            dst_ref=dst,
            send_sem=ssem,
            recv_sem=rsem,
            device_id=(to_ep, to_tp),
            device_id_type=MESH,
        )
        copy.start()
        started.append(copy)

    def arrived(dst, ssem, rsem):
        pltpu.make_async_remote_copy(
            src_ref=dst,
            dst_ref=dst,
            send_sem=ssem,
            recv_sem=rsem,
            device_id=(ep, partner),
            device_id_type=MESH,
        ).wait_recv()

    phase = Phases()
    phase("start")
    load_ow = pltpu.make_async_copy(out_w_hbm, out_w, local_sem.at[0])
    load_eg = pltpu.make_async_copy(eg_hbm.at[0], wgu.at[:, pl.ds(0, ff)], local_sem.at[1])
    load_eu = pltpu.make_async_copy(eu_hbm.at[0], wgu.at[:, pl.ds(ff, ff)], local_sem.at[2])
    load_ed = pltpu.make_async_copy(ed_hbm.at[0], wd, local_sem.at[3])
    load_ow.start()
    load_eg.start()
    load_eu.start()
    load_ed.start()

    barrier = pltpu.get_barrier_semaphore()

    @pl.loop(1, ep_n)
    def _(i):
        pl.semaphore_signal(
            barrier, inc=1, device_id=((ep + i) % ep_n, tp), device_id_type=MESH
        )

    @pl.loop(1, tp_n)
    def _(i):
        pl.semaphore_signal(
            barrier, inc=1, device_id=(ep, (tp + i) % tp_n), device_id_type=MESH
        )

    base = tokens[...].astype(F32)
    scale = lax.rsqrt(jnp.mean(base * base, axis=-1, keepdims=True) + 1e-06)
    gain = mix_gain[...].astype(F32)
    gain2[...] = moe_gain[...].astype(F32)
    for k in range(width // 128):
        piece = base[:, k * 128 : (k + 1) * 128] * scale * gain[k : k + 1, :]
        at = k * 128 % kh
        nrm[k * 128 // kh, :, at : at + 128] = piece.astype(BF16)
    wbuf[0, pl.ds(x * ks, ks), :] = rnn_w[...]
    wbuf[1, pl.ds(x * ks, ks), :] = gate_w[...]
    for h in range(2):
        acts[h, pl.ds(z * rows, rows), :] = nrm[2 * z + h]

    phase("barrier")
    pl.semaphore_wait(barrier, ep_n - 1 + tp_n - 1)
    phase("acts")

    own_w = (rnn_w, gate_w)

    def w_slot(part, xx):
        return wbuf.at[part, pl.ds((xx % NX) * ks, ks), :]

    for n, (part, d) in enumerate(((0, 1), (1, -1), (1, 1), (0, -1))):
        send(
            own_w[part],
            w_slot(part, x),
            w_ssem.at[n],
            w_rsem.at[part, x],
            epid(z, x + d + NX),
            tp,
        )

    order = []
    for i in range(half_z, 0, -1):
        order.append(i)
        if i < half_z:
            order.append(nz - i)
    for i in order:
        to_z = (z + i) % nz
        send(
            nrm.at[2 * to_z + c],
            acts.at[c, pl.ds(z * rows, rows), :],
            a_ssem.at[i],
            a_rsem.at[z],
            epid(to_z, x),
            tp,
        )
    for i in reversed(order):
        from_z = (z + nz - i) % nz
        block = acts.at[c, pl.ds(from_z * rows, rows), :]
        arrived(block, a_ssem.at[i], a_rsem.at[from_z])
        send(block, block, ad_ssem.at[i], ad_rsem.at[from_z], ep, partner)

    phase("weights")
    left = (x + NX - 1) % NX
    right = (x + 1) % NX
    far = (x + 2) % NX
    arrived(w_slot(0, left), w_ssem.at[0], w_rsem.at[0, left])
    send(w_slot(0, left), w_slot(0, left), w_ssem.at[4], w_rsem.at[0, left], epid(z, right), tp)
    arrived(w_slot(1, right), w_ssem.at[0], w_rsem.at[1, right])
    send(w_slot(1, right), w_slot(1, right), w_ssem.at[5], w_rsem.at[1, right], epid(z, left), tp)
    arrived(w_slot(1, left), w_ssem.at[0], w_rsem.at[1, left])
    arrived(w_slot(0, right), w_ssem.at[0], w_rsem.at[0, right])
    for i in reversed(order):
        from_z = (z + nz - i) % nz
        block = acts.at[other, pl.ds(from_z * rows, rows), :]
        arrived(block, ad_ssem.at[i], ad_rsem.at[from_z])
    arrived(w_slot(0, far), w_ssem.at[0], w_rsem.at[0, far])
    arrived(w_slot(1, far), w_ssem.at[0], w_rsem.at[1, far])

    phase("proj")
    for part in range(2):
        pbuf[part] = dot(acts[0], wbuf[part, 0:kh, :]) + dot(acts[1], wbuf[part, kh:kz, :])

    tap = taps[...].astype(F32)
    hist = conv_in[0].astype(F32) * tap[0:1]
    for i in (1, 2):
        conv_out[i - 1] = conv_in[i]
        hist = hist + conv_in[i].astype(F32) * tap[i : i + 1]

    phase("zring")
    chains = ((1, 0, 0), (-1, 1, 0), (1, 1, 1), (-1, 0, 1))

    def part_rows(part, zz):
        return pbuf[part, pl.ds((zz % nz) * rows, rows), :]

    for s in range(half_z):
        for n in (0, 1, 2, 3) if s == 0 else (2, 3, 0, 1):
            d, part, first = chains[n]
            if s < first:
                continue
            value = part_rows(part, z + nz + d * (half_z - s))
            if s > first:
                arrived(rs_recv.at[n, s - 1], rs_ssem.at[n, s], rs_rsem.at[n, s - 1])
                value = value + rs_recv[n, s - 1].astype(F32)
            rs_send[n, s] = value.astype(BF16)
            send(
                rs_send.at[n, s],
                rs_recv.at[n, s],
                rs_ssem.at[n, s],
                rs_rsem.at[n, s],
                epid(z + d + nz, x),
                tp,
            )
    last = half_z - 1
    for n in range(4):
        arrived(rs_recv.at[n, last], rs_ssem.at[n, last], rs_rsem.at[n, last])
    proj_x = part_rows(0, z) + rs_recv[0, last].astype(F32) + rs_recv[3, last].astype(F32)
    proj_y = part_rows(1, z) + rs_recv[1, last].astype(F32) + rs_recv[2, last].astype(F32)

    phase("recur")
    moved = proj_x.astype(BF16)
    conv_out[2] = moved
    conv = (hist + moved.astype(F32) * tap[3:4]).astype(BF16)
    blocks, bw = rate_w.shape[0], rate_w.shape[1]
    rate = jnp.concatenate(
        [dot(conv[:, b * bw : (b + 1) * bw], rate_w[b]) for b in range(blocks)], axis=1
    )
    in_gate = jnp.concatenate(
        [dot(conv[:, b * bw : (b + 1) * bw], input_w[b]) for b in range(blocks)], axis=1
    )
    rate = jax.nn.sigmoid(rate)
    in_gate = jax.nn.sigmoid(in_gate)
    param = rate_param[...]
    soft = jnp.maximum(-param, 0.0) + jnp.log1p(jnp.exp(-jnp.abs(param)))
    log_decay = -8.0 * rate * soft
    tanh_decay = jnp.tanh(log_decay)
    rest = -2.0 * tanh_decay / (1.0 - tanh_decay)
    state = jnp.exp(log_decay) * state_in[...] + jnp.sqrt(rest) * in_gate * conv.astype(F32)
    state_out[...] = state
    gelu = 0.5 * proj_y * (
        1.0 + jnp.tanh(0.7978845608028654 * (proj_y + 0.044715 * proj_y * proj_y * proj_y))
    )
    gated = (state * gelu).astype(BF16)

    phase("outproj")
    load_ow.wait()

    def out_cols(yy, cc):
        return pl.ds(pl.multiple_of(tpid(yy, cc) * chan, chan), chan)

    for i in (2, 1, 3, 0):
        yy = (y + i) % NY
        os_send[i] = dot(gated, out_w[:, out_cols(yy, other)]).astype(BF16)
        send(os_send.at[i], os_recv.at[i], os_ssem.at[i], os_rsem.at[i], ep, partner)
    for i in (2, 1, 3):
        yy = (y + i) % NY
        value = dot(gated, out_w[:, out_cols(yy, c)])
        arrived(os_recv.at[i], os_ssem.at[i], os_rsem.at[i])
        oy_send[i] = (value + os_recv[i].astype(F32)).astype(BF16)
        send(oy_send.at[i], oy_recv.at[i], oy_ssem.at[i], oy_rsem.at[i], ep, tpid(yy, c))
    mixed = tokens[:, out_cols(y, c)].astype(F32) + dot(gated, out_w[:, out_cols(y, c)])

    phase("slots")
    experts = lax.broadcasted_iota(jnp.int32, (ep_n, rows), 0)
    one0 = (routes[0:1, :] == experts).astype(F32)
    one1 = (routes[1:2, :] == experts).astype(F32)
    row_ids = lax.broadcasted_iota(jnp.int32, (rows, rows), 0)
    col_ids = lax.broadcasted_iota(jnp.int32, (rows, rows), 1)
    upper = (row_ids < col_ids).astype(F32).astype(BF16)
    before = dot((one0 + one1).astype(BF16), upper)
    ids = lax.broadcasted_iota(jnp.int32, (2 * slots, rows), 0).astype(F32)

    def one_hot(k, one):
        slot = jnp.sum(before * one, axis=0, keepdims=True)
        first = routes[k : k + 1, :].astype(F32) * (2.0 * cap) + slot
        return (ids == first).astype(F32), (ids == first + cap).astype(F32)

    lo0, hi0 = one_hot(0, one0)
    lo1, hi1 = one_hot(1, one1)
    lo_all = (lo0 + lo1).astype(BF16)
    hi_all = (hi0 + hi1).astype(BF16)

    phase("mixwait")
    arrived(os_recv.at[0], os_ssem.at[0], os_rsem.at[0])
    mixed = mixed + os_recv[0].astype(F32)
    for i in (1, 3, 2):
        arrived(oy_recv.at[i], oy_ssem.at[i], oy_rsem.at[i])
        mixed = mixed + oy_recv[i].astype(F32)
    mixed16 = mixed.astype(BF16)

    phase("dispatch")
    sd[...] = (dot(lo_all, mixed16[:, 0:ch]) + dot(hi_all, mixed16[:, ch:chan])).astype(BF16)
    tile = 2 * cap

    def slot_rows(e):
        return pl.ds(pl.multiple_of(e * tile, tile), tile)

    def scatter(src, dst_of, ssem, rsem):
        @pl.loop(1, ep_n)
        def _(i):
            e = (ep + i) % ep_n
            pltpu.make_async_remote_copy(
                src_ref=src.at[slot_rows(e), :],
                dst_ref=dst_of(ep),
                send_sem=ssem.at[i],
                recv_sem=rsem.at[ep],
                device_id=(e, tp),
                device_id_type=MESH,
            ).start()

    def gathered(src, dst_of, ssem, rsem):
        @pl.loop(1, ep_n)
        def _(i):
            e = (ep + i) % ep_n
            copy = pltpu.make_async_remote_copy(
                src_ref=src.at[slot_rows(e), :],
                dst_ref=dst_of(e),
                send_sem=ssem.at[i],
                recv_sem=rsem.at[e],
                device_id=(e, tp),
                device_id_type=MESH,
            )
            copy.wait_send()
            copy.wait_recv()

    def own_slot(e):
        return gbuf.at[tp, slot_rows(e), :]

    scatter(sd, own_slot, s_ssem, s_rsem)
    gbuf[tp, slot_rows(ep), :] = sd[slot_rows(ep), :]
    phase("loadwait")
    load_eg.wait()
    load_eu.wait()
    load_ed.wait()
    phase("a2a_wait")
    gathered(sd, own_slot, s_ssem, s_rsem)
    phase("ag_own")

    hrows = slots

    def half(t, h):
        return gbuf.at[t, pl.ds(h * hrows, hrows), :]

    counter = [0]

    def share(t, h, to_tp):
        send(half(t, h), half(t, h), ag_ssem.at[counter[0]], ag_rsem.at[t, h], ep, to_tp)
        counter[0] += 1

    def shared(t, h):
        arrived(half(t, h), ag_ssem.at[0], ag_rsem.at[t, h])

    up_tp = tpid(y + 1, c)
    down_tp = tpid(y + 3, c)
    far_tp = tpid(y + 2, c)
    share(tp, 0, up_tp)
    share(tp, 1, down_tp)
    share(tp, 1, up_tp)
    share(tp, 0, down_tp)
    share(tp, 0, partner)
    share(tp, 1, partner)

    squares = jnp.zeros((slots, 1), F32)

    def absorb(t, squares, first):
        value = gbuf[t].astype(F32).reshape(ep_n, 2 * cap, ch)
        parts = (value[:, 0:cap, :], value[:, cap:, :])
        for k in range(2):
            piece = parts[k].reshape(slots, ch)
            squares = squares + jnp.sum(piece * piece, axis=1, keepdims=True)
            at = pl.multiple_of(t * chan + k * ch, ch)
            lanes = []
            for j in range(ch // 128):
                g = gain2[pl.ds(t * (chan // 128) + (k * ch) // 128 + j, 1), :]
                lanes.append((piece[:, j * 128 : (j + 1) * 128] * g).astype(BF16))
            product = dot(jnp.concatenate(lanes, axis=1), wgu[pl.ds(at, ch), :])
            if first and k == 0:
                acc[...] = product
            else:
                acc[...] += product
        return squares

    squares = absorb(tp, squares, True)
    phase("ag_partner")
    shared(partner, 0)
    shared(partner, 1)
    squares = absorb(partner, squares, False)
    phase("ag_near")
    shared(down_tp, 0)
    share(down_tp, 0, up_tp)
    share(down_tp, 0, partner)
    shared(up_tp, 1)
    share(up_tp, 1, down_tp)
    share(up_tp, 1, partner)
    shared(down_tp, 1)
    share(down_tp, 1, partner)
    shared(up_tp, 0)
    share(up_tp, 0, partner)
    phase("absorb_near")
    squares = absorb(down_tp, squares, False)
    squares = absorb(up_tp, squares, False)
    phase("ag_far")
    shared(far_tp, 0)
    share(far_tp, 0, partner)
    shared(far_tp, 1)
    share(far_tp, 1, partner)
    phase("ag_other")
    for i in (3, 1):
        t = tpid(y + i, other)
        shared(t, 0)
        shared(t, 1)
        squares = absorb(t, squares, False)
    phase("ag_last")
    squares = absorb(far_tp, squares, False)
    t = tpid(y + 2, other)
    shared(t, 0)
    shared(t, 1)
    squares = absorb(t, squares, False)

    phase("hidden")
    scale2 = lax.rsqrt(squares * (1.0 / width) + 1e-06)
    gate_part = acc[:, 0:ff] * scale2
    up_part = acc[:, ff:] * scale2
    hidden = (gate_part * jax.nn.sigmoid(gate_part) * up_part).astype(BF16)

    phase("down_send")
    for i in (2, 1, 3, 0):
        d_send[i] = dot(hidden, wd[:, out_cols(y + i, other)]).astype(BF16)
        send(d_send.at[i], d_recv.at[i], d_ssem.at[i], d_rsem.at[i], ep, partner)

    hs = slots // 2

    def own_part(i):
        value = dot(hidden, wd[:, out_cols(y + i, c)])
        arrived(d_recv.at[i], d_ssem.at[i], d_rsem.at[i])
        return value + d_recv[i].astype(F32)

    phase("down_own")
    value = own_part(2)
    q_send[0] = value[0:hs].astype(BF16)
    send(q_send.at[0], fw_recv.at[0], q_ssem.at[0], fw_rsem.at[0], ep, up_tp)
    q_send[1] = value[hs:].astype(BF16)
    send(q_send.at[1], fw_recv.at[1], q_ssem.at[1], fw_rsem.at[1], ep, down_tp)
    value = own_part(1)
    q_send[2] = value[hs:].astype(BF16)
    send(q_send.at[2], fin_recv.at[0, 1], q_ssem.at[2], fin_rsem.at[0, 1], ep, up_tp)
    qf[0] = value[0:hs]
    value = own_part(3)
    q_send[3] = value[0:hs].astype(BF16)
    send(q_send.at[3], fin_recv.at[1, 0], q_ssem.at[3], fin_rsem.at[1, 0], ep, down_tp)
    qf[1] = value[hs:]
    phase("rs_fw")
    arrived(fw_recv.at[0], q_ssem.at[0], fw_rsem.at[0])
    q_send[4] = (qf[0] + fw_recv[0].astype(F32)).astype(BF16)
    send(q_send.at[4], fin_recv.at[0, 0], q_ssem.at[4], fin_rsem.at[0, 0], ep, up_tp)
    arrived(fw_recv.at[1], q_ssem.at[0], fw_rsem.at[1])
    q_send[5] = (qf[1] + fw_recv[1].astype(F32)).astype(BF16)
    send(q_send.at[5], fin_recv.at[1, 1], q_ssem.at[5], fin_rsem.at[1, 1], ep, down_tp)
    phase("rs_fin")
    value = own_part(0)
    for h in range(2):
        total = value[h * hs : (h + 1) * hs]
        for d in range(2):
            arrived(fin_recv.at[d, h], q_ssem.at[0], fin_rsem.at[d, h])
            total = total + fin_recv[d, h].astype(F32)
        total = total.reshape(hs // cap, cap, chan)
        total = jnp.concatenate([total[:, :, 0:ch], total[:, :, ch:]], axis=1)
        back_send[h * slots : (h + 1) * slots, :] = total.reshape(slots, ch).astype(BF16)

    phase("back")
    def back_slot(e):
        return back_recv.at[slot_rows(e), :]

    scatter(back_send, back_slot, b_ssem, b_rsem)
    back_recv[slot_rows(ep), :] = back_send[slot_rows(ep), :]
    total = prob[0:1, :] + prob[1:2, :]
    eye = row_ids == col_ids

    def column(row):
        return jnp.sum(jnp.where(eye, row, 0.0), axis=1, keepdims=True)

    w0 = column(prob[0:1, :] / total)
    w1 = column(prob[1:2, :] / total)
    phase("back_wait")
    gathered(back_send, back_slot, b_ssem, b_rsem)
    phase("combine")
    returned = back_recv[...]
    for k, (a, b) in enumerate(((lo0, lo1), (hi0, hi1))):
        picked = w0 * dot_t(a.astype(BF16), returned) + w1 * dot_t(b.astype(BF16), returned)
        layer_out[:, k * ch : (k + 1) * ch] = (
            mixed[:, k * ch : (k + 1) * ch] + picked
        ).astype(BF16)

    phase("drain")
    for copy in started:
        copy.wait_send()
    phase(None)


def shards(
    tokens,
    state_in,
    conv_in,
    mix_gain,
    rnn_weight,
    gate_weight,
    conv_weight,
    rate_weight,
    input_weight,
    rate_param,
    out_weight,
    moe_gain,
    expert_gate,
    expert_up,
    expert_down,
    routes,
    route_prob,
):
    rows, width = tokens.shape
    ks, chan = rnn_weight.shape
    ep_n = lax.axis_size("ep")
    tp_n = lax.axis_size("tp")
    nz = ep_n // NX
    half_z = nz // 2
    kh = width // nz // 2
    ff = expert_down.shape[1]
    topk = routes.shape[1]
    cap = max(2, 2 * rows * topk // ep_n)
    slots = ep_n * cap
    ch = chan // 2

    vm = pl.BlockSpec(memory_space=pltpu.VMEM)
    hbm = pl.BlockSpec(memory_space=pl.ANY)
    dma = pltpu.SemaphoreType.DMA
    layer_out, state_out, conv_out = pl.pallas_call(
        layer_kernel,
        out_shape=(
            jax.ShapeDtypeStruct((rows, chan), BF16),
            jax.ShapeDtypeStruct((rows, chan), F32),
            jax.ShapeDtypeStruct((3, rows, chan), BF16),
        ),
        in_specs=[vm] * 13 + [hbm] * 4,
        out_specs=(vm, vm, vm),
        scratch_shapes=[
            pltpu.VMEM((chan, width), BF16),
            pltpu.VMEM((width, 2 * ff), BF16),
            pltpu.VMEM((ff, width), BF16),
            pltpu.VMEM((2 * nz, rows, kh), BF16),
            pltpu.VMEM((2, nz * rows, kh), BF16),
            pltpu.VMEM((2, NX * ks, chan), BF16),
            pltpu.VMEM((2, nz * rows, chan), F32),
            pltpu.VMEM((4, half_z, rows, chan), BF16),
            pltpu.VMEM((4, half_z, rows, chan), BF16),
            pltpu.VMEM((NY, rows, chan), BF16),
            pltpu.VMEM((NY, rows, chan), BF16),
            pltpu.VMEM((NY, rows, chan), BF16),
            pltpu.VMEM((NY, rows, chan), BF16),
            pltpu.VMEM((2 * slots, ch), BF16),
            pltpu.VMEM((tp_n, 2 * slots, ch), BF16),
            pltpu.VMEM((width // 128, 128), F32),
            pltpu.VMEM((slots, 2 * ff), F32),
            pltpu.VMEM((NY, slots, chan), BF16),
            pltpu.VMEM((NY, slots, chan), BF16),
            pltpu.VMEM((2, slots // 2, chan), F32),
            pltpu.VMEM((6, slots // 2, chan), BF16),
            pltpu.VMEM((2, slots // 2, chan), BF16),
            pltpu.VMEM((2, 2, slots // 2, chan), BF16),
            pltpu.VMEM((2 * slots, ch), BF16),
            pltpu.VMEM((2 * slots, ch), BF16),
            dma((4,)),
            dma((6,)),
            dma((2, NX)),
            dma((nz,)),
            dma((nz,)),
            dma((nz,)),
            dma((nz,)),
            dma((4, half_z)),
            dma((4, half_z)),
            dma((NY,)),
            dma((NY,)),
            dma((NY,)),
            dma((NY,)),
            dma((ep_n,)),
            dma((ep_n,)),
            dma((14,)),
            dma((tp_n, 2)),
            dma((NY,)),
            dma((NY,)),
            dma((6,)),
            dma((2,)),
            dma((2, 2)),
            dma((ep_n,)),
            dma((ep_n,)),
        ],
        compiler_params=pltpu.CompilerParams(
            collective_id=0,
            has_side_effects=True,
            vmem_limit_bytes=60 * 1024 * 1024,
        ),
        name="layer",
    )(
        tokens,
        conv_in.transpose(1, 0, 2),
        state_in,
        mix_gain.reshape(width // 128, 128),
        rnn_weight,
        gate_weight,
        conv_weight,
        rate_weight,
        input_weight,
        rate_param.reshape(1, chan),
        moe_gain.reshape(width // 128, 128),
        routes.T,
        route_prob.T,
        out_weight,
        expert_gate,
        expert_up,
        expert_down,
    )
    return (layer_out, state_out, conv_out.transpose(1, 0, 2))


def solution(mesh):
    in_specs = (
        P("ep", None),
        P("ep", "tp"),
        P("ep", None, "tp"),
        P(),
        P("ep", "tp"),
        P("ep", "tp"),
        P(None, "tp"),
        P("tp", None, None),
        P("tp", None, None),
        P("tp"),
        P("tp", None),
        P(),
        P("ep", None, "tp"),
        P("ep", None, "tp"),
        P("ep", "tp", None),
        P("ep", None),
        P("ep", None),
    )
    out_specs = (P("ep", "tp"), P("ep", "tp"), P("ep", None, "tp"))
    return jax.shard_map(shards, mesh=mesh, in_specs=in_specs, out_specs=out_specs, check_vma=False)
```

```python
import functools

import jax
import jax.numpy as jnp
from jax import lax
from jax.experimental import pallas as pl
from jax.experimental.pallas import tpu as pltpu
from jax.sharding import PartitionSpec as P

NX = 4
NY = 4
NC = 2
MESH = pl.DeviceIdType.MESH
F32 = jnp.float32
BF16 = jnp.bfloat16


def dot(a, b):
    return jnp.dot(a, b, preferred_element_type=F32)


def dot_t(a, b):
    return lax.dot_general(a, b, (((0,), (0,)), ((), ())), preferred_element_type=F32)


class Phases:
    def __init__(self):
        self.scope = None

    def __call__(self, name):
        if self.scope is not None:
            self.scope.__exit__(None, None, None)
        self.scope = jax.named_scope(name) if name else None
        if self.scope is not None:
            self.scope.__enter__()


def layer_kernel(
    tokens_hbm,
    conv_in_hbm,
    state_in_hbm,
    mix_gain_hbm,
    rnn_w_hbm,
    gate_w_hbm,
    taps_hbm,
    rate_w_hbm,
    input_w_hbm,
    rate_param_hbm,
    moe_gain_hbm,
    routes_hbm,
    prob_hbm,
    out_w_hbm,
    eg_hbm,
    eu_hbm,
    ed_hbm,
    layer_out,
    state_out,
    conv_out,
    tokens,
    conv_in,
    state_in,
    mix_gain,
    taps,
    rate_w,
    input_w,
    rate_param,
    moe_gain,
    routes,
    prob,
    out_w,
    wgu,
    wd,
    nrm,
    acts,
    wbuf,
    pbuf,
    rs_send,
    rs_recv,
    os_send,
    os_recv,
    oy_send,
    oy_recv,
    sd,
    gbuf,
    gain2,
    acc,
    d_send,
    d_recv,
    qf,
    q_send,
    fw_recv,
    fin_recv,
    back_send,
    back_recv,
    local_sem,
    w_ssem,
    w_rsem,
    a_ssem,
    a_rsem,
    ad_ssem,
    ad_rsem,
    rs_ssem,
    rs_rsem,
    os_ssem,
    os_rsem,
    oy_ssem,
    oy_rsem,
    s_ssem,
    s_rsem,
    ag_ssem,
    ag_rsem,
    ao_rsem,
    d_ssem,
    d_rsem,
    q_ssem,
    fw_rsem,
    fin_rsem,
    b_ssem,
    b_rsem,
):
    rows, width = tokens.shape
    ks, chan = rnn_w_hbm.shape
    ep_n = width // ks
    nz = ep_n // NX
    half_z = nz // 2
    tp_n = NY * NC
    kz = width // nz
    kh = kz // 2
    ff = wd.shape[0]
    cap = sd.shape[0] // ep_n // 2
    ch = chan // 2
    slots = ep_n * cap

    ep = lax.axis_index("ep")
    tp = lax.axis_index("tp")
    z = ep // NX
    x = ep % NX
    y = tp // NC
    c = tp % NC
    other = (c + 1) % NC

    def epid(zz, xx):
        return (zz % nz) * NX + xx % NX

    def tpid(yy, cc):
        return (yy % NY) * NC + cc

    partner = tpid(y, other)

    def send(src, dst, ssem, rsem, to_ep, to_tp):
        copy = pltpu.make_async_remote_copy(
            src_ref=src,
            dst_ref=dst,
            send_sem=ssem,
            recv_sem=rsem,
            device_id=(to_ep, to_tp),
            device_id_type=MESH,
        )
        copy.start()

    def arrived(dst, ssem, rsem):
        pltpu.make_async_remote_copy(
            src_ref=dst,
            dst_ref=dst,
            send_sem=ssem,
            recv_sem=rsem,
            device_id=(ep, partner),
            device_id_type=MESH,
        ).wait_recv()

    def sent(src, ssem, rsem):
        pltpu.make_async_remote_copy(
            src_ref=src,
            dst_ref=src,
            send_sem=ssem,
            recv_sem=rsem,
            device_id=(ep, partner),
            device_id_type=MESH,
        ).wait_send()

    phase = Phases()
    phase("start")

    barrier = pltpu.get_barrier_semaphore()

    @pl.loop(1, ep_n)
    def _(i):
        pl.semaphore_signal(
            barrier, inc=1, device_id=((ep + i) % ep_n, tp), device_id_type=MESH
        )

    @pl.loop(1, tp_n)
    def _(i):
        pl.semaphore_signal(
            barrier, inc=1, device_id=(ep, (tp + i) % tp_n), device_id_type=MESH
        )

    def own_rows(part):
        return wbuf.at[part, pl.ds(x * ks, ks), :]

    loads = {}
    for n, (name, src, dst) in enumerate(
        (
            ("tokens", tokens_hbm, tokens),
            ("mix_gain", mix_gain_hbm, mix_gain),
            ("rnn_w", rnn_w_hbm, own_rows(0)),
            ("gate_w", gate_w_hbm, own_rows(1)),
            ("moe_gain", moe_gain_hbm, moe_gain),
            ("conv_in", conv_in_hbm, conv_in),
            ("taps", taps_hbm, taps),
            ("rate_w", rate_w_hbm, rate_w),
            ("input_w", input_w_hbm, input_w),
            ("rate_param", rate_param_hbm, rate_param),
            ("state_in", state_in_hbm, state_in),
            ("routes", routes_hbm, routes),
            ("prob", prob_hbm, prob),
            ("out_w", out_w_hbm, out_w),
            ("eg", eg_hbm.at[0], wgu.at[:, pl.ds(0, ff)]),
            ("eu", eu_hbm.at[0], wgu.at[:, pl.ds(ff, ff)]),
            ("ed", ed_hbm.at[0], wd),
        )
    ):
        loads[name] = pltpu.make_async_copy(src, dst, local_sem.at[n])
        loads[name].start()

    loads["tokens"].wait()
    loads["mix_gain"].wait()
    base = tokens[...].astype(F32)
    scale = lax.rsqrt(jnp.mean(base * base, axis=-1, keepdims=True) + 1e-06)
    gain = mix_gain[...].astype(F32)
    for k in range(width // 128):
        piece = base[:, k * 128 : (k + 1) * 128] * scale * gain[k : k + 1, :]
        at = k * 128 % kh
        nrm[k * 128 // kh, :, at : at + 128] = piece.astype(BF16)
    for h in range(2):
        acts[h, pl.ds(z * rows, rows), :] = nrm[2 * z + h]
    loads["rnn_w"].wait()
    loads["gate_w"].wait()

    phase("barrier")
    pl.semaphore_wait(barrier, ep_n - 1 + tp_n - 1)
    phase("acts")

    left = (x + NX - 1) % NX
    right = (x + 1) % NX
    far = (x + 2) % NX
    hk = ks // 2

    def w_slot(part, xx, h):
        return wbuf.at[part, pl.ds(xx * ks + h * hk, hk), :]

    def w_send(part, xx, h, to_x):
        slot = w_slot(part, xx, h)
        send(slot, slot, w_ssem.at[part], w_rsem.at[part, xx, h], epid(z, to_x), tp)

    def w_wait(part, xx, h):
        arrived(w_slot(part, xx, h), w_ssem.at[part], w_rsem.at[part, xx, h])

    def w_direct(part):
        w_send(part, x, 0, right)
        w_send(part, x, 1, left)
        w_send(part, x, 1, right)
        w_send(part, x, 0, left)

    def w_forward(part):
        w_wait(part, left, 0)
        w_send(part, left, 0, right)
        w_wait(part, right, 1)
        w_send(part, right, 1, left)

    def w_rest(part):
        w_wait(part, left, 1)
        w_wait(part, right, 0)
        w_wait(part, far, 0)
        w_wait(part, far, 1)

    w_direct(0)

    order = []
    for i in range(half_z, 0, -1):
        order.append(i)
        if i < half_z:
            order.append(nz - i)
    for i in order:
        to_z = (z + i) % nz
        send(
            nrm.at[2 * to_z + c],
            acts.at[c, pl.ds(z * rows, rows), :],
            a_ssem.at[0],
            a_rsem.at[z],
            epid(to_z, x),
            tp,
        )

    def act_block(cc, i):
        return acts.at[cc, pl.ds((z + nz - i) % nz * rows, rows), :]

    def act_pass(i):
        block = act_block(c, i)
        from_z = (z + nz - i) % nz
        arrived(block, a_ssem.at[0], a_rsem.at[from_z])
        send(block, block, ad_ssem.at[0], ad_rsem.at[0], ep, partner)

    w_forward(0)
    w_direct(1)
    phase("acts2")
    for i in order[::-1]:
        act_pass(i)
    phase("weights")
    w_rest(0)
    phase("acts_other")
    arrived(nrm.at[pl.ds(0, nz - 1)], ad_ssem.at[0], ad_rsem.at[0])

    phase("proj0")

    def project(part):
        pbuf[part] = dot(acts[0], wbuf[part, 0:kh, :]) + dot(acts[1], wbuf[part, kh:kz, :])

    chains = ((1, 0, 0), (-1, 0, 1), (-1, 1, 0), (1, 1, 1))
    last = half_z - 1

    def part_rows(part, zz):
        return pbuf[part, pl.ds((zz % nz) * rows, rows), :]

    def ring(n, s):
        d, part, first = chains[n]
        value = part_rows(part, z + nz + d * (half_z - s))
        if s > first:
            arrived(rs_recv.at[n, s - 1], rs_ssem.at[n], rs_rsem.at[n, s - 1])
            value = value + rs_recv[n, s - 1].astype(F32)
        rs_send[n, s] = value.astype(BF16)
        send(
            rs_send.at[n, s],
            rs_recv.at[n, s],
            rs_ssem.at[n],
            rs_rsem.at[n, s],
            epid(z + d + nz, x),
            tp,
        )

    def ring_end(part):
        value = part_rows(part, z)
        for n in (2 * part, 2 * part + 1):
            arrived(rs_recv.at[n, last], rs_ssem.at[n], rs_rsem.at[n, last])
            value = value + rs_recv[n, last].astype(F32)
        return value

    project(0)
    ring(0, 0)
    ring(1, 1)
    phase("w1")
    w_forward(1)
    phase("ring0a")
    ring(0, 1)
    phase("w1rest")
    w_rest(1)
    phase("proj1")
    project(1)
    ring(2, 0)
    ring(3, 1)
    phase("ring2")
    for s in range(2, half_z):
        ring(1, s)
        ring(0, s)
        ring(2, s - 1)
        if s > 2:
            ring(3, s - 1)
    phase("local")
    loads["conv_in"].wait()
    loads["taps"].wait()
    loads["moe_gain"].wait()
    gain2[...] = moe_gain[...].astype(F32)
    tap = taps[...].astype(F32)
    hist = conv_in[0].astype(F32) * tap[0:1]
    for i in (1, 2):
        conv_out[i - 1] = conv_in[i]
        hist = hist + conv_in[i].astype(F32) * tap[i : i + 1]
    loads["routes"].wait()
    loads["prob"].wait()

    phase("ring3")
    proj_x = ring_end(0)
    ring(3, last)
    ring(2, last)

    phase("recur")
    moved = proj_x.astype(BF16)
    conv_out[2] = moved
    conv = (hist + moved.astype(F32) * tap[3:4]).astype(BF16)
    for name in ("rate_w", "input_w", "rate_param", "state_in"):
        loads[name].wait()
    blocks, bw = rate_w.shape[0], rate_w.shape[1]
    rate = jnp.concatenate(
        [dot(conv[:, b * bw : (b + 1) * bw], rate_w[b]) for b in range(blocks)], axis=1
    )
    in_gate = jnp.concatenate(
        [dot(conv[:, b * bw : (b + 1) * bw], input_w[b]) for b in range(blocks)], axis=1
    )
    rate = jax.nn.sigmoid(rate)
    in_gate = jax.nn.sigmoid(in_gate)
    param = rate_param[...]
    soft = jnp.maximum(-param, 0.0) + jnp.log1p(jnp.exp(-jnp.abs(param)))
    log_decay = -8.0 * rate * soft
    tanh_decay = jnp.tanh(log_decay)
    rest = -2.0 * tanh_decay / (1.0 - tanh_decay)
    state = jnp.exp(log_decay) * state_in[...] + jnp.sqrt(rest) * in_gate * conv.astype(F32)
    state_out[...] = state
    phase("ring4")
    proj_y = ring_end(1)
    gelu = 0.5 * proj_y * (
        1.0 + jnp.tanh(0.7978845608028654 * (proj_y + 0.044715 * proj_y * proj_y * proj_y))
    )
    gated = (state * gelu).astype(BF16)

    phase("outproj")
    loads["out_w"].wait()

    def out_cols(yy, cc):
        return pl.ds(pl.multiple_of(tpid(yy, cc) * chan, chan), chan)

    for i in (2, 1, 3, 0):
        os_send[i] = dot(gated, out_w[:, out_cols(y + i, other)]).astype(BF16)
        send(os_send.at[i], os_recv.at[i], os_ssem.at[0], os_rsem.at[i], ep, partner)
    for i in (2, 1, 3):
        value = dot(gated, out_w[:, out_cols(y + i, c)])
        arrived(os_recv.at[i], os_ssem.at[0], os_rsem.at[i])
        oy_send[i] = (value + os_recv[i].astype(F32)).astype(BF16)
        send(oy_send.at[i], oy_recv.at[i], oy_ssem.at[0], oy_rsem.at[i], ep, tpid(y + i, c))
    mixed = tokens[:, out_cols(y, c)].astype(F32) + dot(gated, out_w[:, out_cols(y, c)])

    phase("slots")

    def place(dz):
        return jnp.where(dz <= half_z, jnp.maximum(2 * dz - 1, 0), 2 * (nz - dz))

    offsets = [0]
    for i in range(1, half_z + 1):
        offsets.append(i)
        if i < half_z:
            offsets.append(nz - i)

    experts = lax.broadcasted_iota(jnp.int32, (ep_n, rows), 0)
    chosen = [routes[k : k + 1, :] for k in range(2)]
    one0 = (chosen[0] == experts).astype(F32)
    one1 = (chosen[1] == experts).astype(F32)
    row_ids = lax.broadcasted_iota(jnp.int32, (rows, rows), 0)
    col_ids = lax.broadcasted_iota(jnp.int32, (rows, rows), 1)
    upper = (row_ids < col_ids).astype(F32).astype(BF16)
    before = dot((one0 + one1).astype(BF16), upper)
    ids = lax.broadcasted_iota(jnp.int32, (2 * slots, rows), 0).astype(F32)

    def one_hot(e, one):
        slot = jnp.sum(before * one, axis=0, keepdims=True)
        dz = e // NX - z
        dz = jnp.where(dz < 0, dz + nz, dz)
        block = place(dz) * NX + e % NX
        first = block.astype(F32) * (2.0 * cap) + slot
        return (ids == first).astype(F32), (ids == first + cap).astype(F32)

    lo0, hi0 = one_hot(chosen[0], one0)
    lo1, hi1 = one_hot(chosen[1], one1)
    lo_all = (lo0 + lo1).astype(BF16)
    hi_all = (hi0 + hi1).astype(BF16)

    phase("mixwait")
    arrived(os_recv.at[0], os_ssem.at[0], os_rsem.at[0])
    mixed = mixed + os_recv[0].astype(F32)
    for i in (1, 3, 2):
        arrived(oy_recv.at[i], oy_ssem.at[0], oy_rsem.at[i])
        mixed = mixed + oy_recv[i].astype(F32)
    mixed16 = mixed.astype(BF16)

    phase("dispatch")
    tile = 2 * cap
    per = nz // 2

    def tile_rows(block):
        return pl.ds(pl.multiple_of(block * tile, tile), tile)

    def scatter(g, src, dst, ssem, rsem, sign):
        for j in range(g * per, (g + 1) * per):
            for i in range(NX):
                if j == 0 and i == 0:
                    continue
                to_x = (x + i) % NX
                send(
                    src.at[tile_rows(j * NX + to_x), :],
                    dst.at[tile_rows(j * NX + x), :],
                    ssem.at[0],
                    rsem.at[g],
                    epid(z + nz + sign * offsets[j], to_x),
                    tp,
                )

    def gathered(g, dst, ssem, rsem):
        start = tile if g == 0 else slots
        arrived(dst.at[pl.ds(start, (g + 1) * slots - start), :], ssem.at[0], rsem.at[g])

    def scattered(src, ssem, rsem):
        sent(src.at[pl.ds(tile, 2 * slots - tile), :], ssem.at[0], rsem.at[0])

    for g in range(2):
        part = slice(g * slots, (g + 1) * slots)
        sd[part, :] = (
            dot(lo_all[part], mixed16[:, 0:ch]) + dot(hi_all[part], mixed16[:, ch:chan])
        ).astype(BF16)
        scatter(g, sd, gbuf.at[tp], s_ssem, s_rsem, 1)
    gbuf[tp, tile_rows(x), :] = sd[tile_rows(x), :]

    hs = slots // 2

    def piece_of(t, g, q):
        return gbuf.at[t, pl.ds(g * slots + q * hs, hs), :]

    def share(t, g, q, to_tp):
        ref = piece_of(t, g, q)
        rsem = ao_rsem.at[t // NC, g] if to_tp is partner else ag_rsem.at[t // NC, g, q]
        send(ref, ref, ag_ssem.at[g], rsem, ep, to_tp)

    def shared(t, g, q):
        arrived(piece_of(t, g, q), ag_ssem.at[g], ag_rsem.at[t // NC, g, q])

    def shared_other(t, g):
        both = gbuf.at[t, pl.ds(g * slots, slots), :]
        arrived(both, ag_ssem.at[g], ao_rsem.at[t // NC, g])

    up_tp = tpid(y + 1, c)
    down_tp = tpid(y + 3, c)
    far_tp = tpid(y + 2, c)

    def own_share(g):
        share(tp, g, 0, up_tp)
        share(tp, g, 1, down_tp)
        share(tp, g, 1, up_tp)
        share(tp, g, 0, down_tp)
        share(tp, g, 0, partner)
        share(tp, g, 1, partner)

    def near_share(g):
        shared(down_tp, g, 0)
        share(down_tp, g, 0, up_tp)
        share(down_tp, g, 0, partner)
        shared(up_tp, g, 1)
        share(up_tp, g, 1, down_tp)
        share(up_tp, g, 1, partner)
        shared(down_tp, g, 1)
        share(down_tp, g, 1, partner)
        shared(up_tp, g, 0)
        share(up_tp, g, 0, partner)

    def far_share(g):
        for q in range(2):
            shared(far_tp, g, q)
            share(far_tp, g, q, partner)

    squares = [jnp.zeros((hs, 1), F32), jnp.zeros((hs, 1), F32)]

    def absorb(t, g, first=False):
        value = gbuf[t, g * slots : (g + 1) * slots, :].astype(F32)
        value = value.reshape(ep_n // 2, tile, ch)
        parts = (value[:, 0:cap, :], value[:, cap:, :])
        for k in range(2):
            piece = parts[k].reshape(hs, ch)
            squares[g] = squares[g] + jnp.sum(piece * piece, axis=1, keepdims=True)
            lanes = []
            for j in range(ch // 128):
                row = gain2[pl.ds(t * (chan // 128) + (k * ch) // 128 + j, 1), :]
                lanes.append((piece[:, j * 128 : (j + 1) * 128] * row).astype(BF16))
            at = pl.multiple_of(t * chan + k * ch, ch)
            product = dot(jnp.concatenate(lanes, axis=1), wgu[pl.ds(at, ch), :])
            if first and k == 0:
                acc[g] = product
            else:
                acc[g] += product

    def absorb_other(i, g):
        t = tpid(y + i, other)
        shared_other(t, g)
        absorb(t, g)

    def hidden_of(g):
        scale2 = lax.rsqrt(squares[g] * (1.0 / width) + 1e-06)
        gate_part = acc[g, :, 0:ff] * scale2
        up_part = acc[g, :, ff:] * scale2
        return (gate_part * jax.nn.sigmoid(gate_part) * up_part).astype(BF16)

    hq = hs // 2

    def down_send(g, hidden):
        for i in (2, 1, 3, 0):
            d_send[g, i] = dot(hidden, wd[:, out_cols(y + i, other)]).astype(BF16)
            send(d_send.at[g, i], d_recv.at[g, i], d_ssem.at[g], d_rsem.at[g, i], ep, partner)

    def own_part(g, hidden, i):
        value = dot(hidden, wd[:, out_cols(y + i, c)])
        arrived(d_recv.at[g, i], d_ssem.at[g], d_rsem.at[g, i])
        return value + d_recv[g, i].astype(F32)

    def q_out(g, n, value, dst, rsem, to_tp):
        q_send[g, n] = value.astype(BF16)
        send(q_send.at[g, n], dst, q_ssem.at[g], rsem, ep, to_tp)

    def rs_first(g, hidden):
        value = own_part(g, hidden, 2)
        q_out(g, 0, value[0:hq], fw_recv.at[g, 0], fw_rsem.at[g, 0], up_tp)
        q_out(g, 1, value[hq:], fw_recv.at[g, 1], fw_rsem.at[g, 1], down_tp)
        value = own_part(g, hidden, 1)
        q_out(g, 2, value[hq:], fin_recv.at[g, 1, 0], fin_rsem.at[g, 1], up_tp)
        qf[g, 0] = value[0:hq]
        value = own_part(g, hidden, 3)
        q_out(g, 3, value[0:hq], fin_recv.at[g, 0, 1], fin_rsem.at[g, 0], down_tp)
        qf[g, 1] = value[hq:]
        qf[g, 2] = own_part(g, hidden, 0)[0:hq]
        qf[g, 3] = own_rest(g, hidden)

    def own_rest(g, hidden):
        return dot(hidden[hq:], wd[:, out_cols(y, c)]) + d_recv[g, 0, hq:, :].astype(F32)

    def rs_forward(g):
        arrived(fw_recv.at[g, 0], q_ssem.at[g], fw_rsem.at[g, 0])
        value = qf[g, 0] + fw_recv[g, 0].astype(F32)
        q_out(g, 4, value, fin_recv.at[g, 0, 0], fin_rsem.at[g, 0], up_tp)
        arrived(fw_recv.at[g, 1], q_ssem.at[g], fw_rsem.at[g, 1])
        value = qf[g, 1] + fw_recv[g, 1].astype(F32)
        q_out(g, 5, value, fin_recv.at[g, 1, 1], fin_rsem.at[g, 1], down_tp)

    def rs_final(g):
        for h in range(2):
            arrived(fin_recv.at[g, h], q_ssem.at[g], fin_rsem.at[g, h])
            total = qf[g, 2 + h] + fin_recv[g, h, 0].astype(F32) + fin_recv[g, h, 1].astype(F32)
            total = total.reshape(hq // cap, cap, chan)
            total = jnp.concatenate([total[:, :, 0:ch], total[:, :, ch:]], axis=1)
            at = g * slots + h * hs
            back_send[at : at + hs, :] = total.reshape(hs, ch).astype(BF16)

    phase("a2a_wait0")
    gathered(0, gbuf.at[tp], s_ssem, s_rsem)
    own_share(0)
    phase("absorb0")
    loads["eg"].wait()
    loads["eu"].wait()
    loads["ed"].wait()
    absorb(tp, 0, True)
    absorb_other(0, 0)
    phase("near0")
    near_share(0)
    phase("a2a_wait1")
    gathered(1, gbuf.at[tp], s_ssem, s_rsem)
    own_share(1)
    phase("absorb_near0")
    absorb(down_tp, 0)
    absorb(up_tp, 0)
    phase("far0")
    far_share(0)
    phase("other0")
    absorb_other(3, 0)
    absorb_other(1, 0)
    absorb(far_tp, 0)
    absorb_other(2, 0)
    phase("hidden0")
    hidden0 = hidden_of(0)
    down_send(0, hidden0)
    phase("near1")
    near_share(1)
    phase("rs_first0")
    rs_first(0, hidden0)
    phase("absorb1")
    absorb(tp, 1, True)
    absorb_other(0, 1)
    absorb(down_tp, 1)
    absorb(up_tp, 1)
    phase("far1")
    far_share(1)
    phase("other1")
    absorb_other(3, 1)
    absorb_other(1, 1)
    absorb(far_tp, 1)
    absorb_other(2, 1)
    phase("hidden1")
    hidden1 = hidden_of(1)
    down_send(1, hidden1)
    phase("rs_fw0")
    rs_forward(0)
    phase("rs_first1")
    rs_first(1, hidden1)
    phase("rs_fin0")
    rs_final(0)
    scatter(0, back_send, back_recv, b_ssem, b_rsem, -1)
    phase("rs_fw1")
    rs_forward(1)
    back_recv[tile_rows(x), :] = back_send[tile_rows(x), :]
    total = prob[0:1, :] + prob[1:2, :]
    eye = row_ids == col_ids

    def column(row):
        return jnp.sum(jnp.where(eye, row, 0.0), axis=1, keepdims=True)

    w0 = column(prob[0:1, :] / total)
    w1 = column(prob[1:2, :] / total)
    phase("rs_fin1")
    rs_final(1)
    scatter(1, back_send, back_recv, b_ssem, b_rsem, -1)
    phase("back_wait0")
    gathered(0, back_recv, b_ssem, b_rsem)
    phase("back_wait1")
    gathered(1, back_recv, b_ssem, b_rsem)
    phase("combine")
    returned = back_recv[...]
    for k, (a, b) in enumerate(((lo0, lo1), (hi0, hi1))):
        picked = w0 * dot_t(a.astype(BF16), returned) + w1 * dot_t(b.astype(BF16), returned)
        layer_out[:, k * ch : (k + 1) * ch] = (
            mixed[:, k * ch : (k + 1) * ch] + picked
        ).astype(BF16)

    phase("drain")
    for part in range(2):
        sent(wbuf.at[part, pl.ds(0, 6 * hk), :], w_ssem.at[part], w_rsem.at[part, 0, 0])
    sent(nrm.at[pl.ds(0, nz - 1)], a_ssem.at[0], a_rsem.at[0])
    sent(nrm.at[pl.ds(0, nz - 1)], ad_ssem.at[0], ad_rsem.at[0])
    for n in range(4):
        first = chains[n][2]
        sent(rs_send.at[n, pl.ds(first, half_z - first)], rs_ssem.at[n], rs_rsem.at[n, 0])
    sent(os_send, os_ssem.at[0], os_rsem.at[0])
    sent(oy_send.at[pl.ds(1, NY - 1)], oy_ssem.at[0], oy_rsem.at[0])
    scattered(sd, s_ssem, s_rsem)
    for g in range(2):
        sent(gbuf.at[pl.ds(0, 7), pl.ds(0, slots), :], ag_ssem.at[g], ag_rsem.at[0, g, 0])
        sent(d_send.at[g], d_ssem.at[g], d_rsem.at[g, 0])
        sent(q_send.at[g], q_ssem.at[g], fw_rsem.at[g, 0])
    scattered(back_send, b_ssem, b_rsem)
    phase(None)


def finish_kernel(a, b, c, a_out, b_out, c_out, sems):
    copies = [
        pltpu.make_async_copy(src, dst, sems.at[n])
        for n, (src, dst) in enumerate(((a, a_out), (b, b_out), (c, c_out)))
    ]
    for copy in copies:
        copy.start()
    for copy in copies:
        copy.wait()


def shards(
    tokens,
    state_in,
    conv_in,
    mix_gain,
    rnn_weight,
    gate_weight,
    conv_weight,
    rate_weight,
    input_weight,
    rate_param,
    out_weight,
    moe_gain,
    expert_gate,
    expert_up,
    expert_down,
    routes,
    route_prob,
):
    rows, width = tokens.shape
    ks, chan = rnn_weight.shape
    ep_n = lax.axis_size("ep")
    tp_n = lax.axis_size("tp")
    nz = ep_n // NX
    half_z = nz // 2
    kh = width // nz // 2
    ff = expert_down.shape[1]
    topk = routes.shape[1]
    cap = max(2, 2 * rows * topk // ep_n)
    slots = ep_n * cap
    hs = slots // 2
    ch = chan // 2

    vm = pl.BlockSpec(memory_space=pltpu.VMEM)
    hbm = pl.BlockSpec(memory_space=pltpu.HBM)
    dma = pltpu.SemaphoreType.DMA
    shapes = (
        jax.ShapeDtypeStruct((rows, chan), BF16),
        jax.ShapeDtypeStruct((rows, chan), F32),
        jax.ShapeDtypeStruct((3, rows, chan), BF16),
    )
    outs = pl.pallas_call(
        layer_kernel,
        out_shape=tuple(pltpu.VMEM(a.shape, a.dtype) for a in shapes),
        in_specs=[hbm] * 17,
        out_specs=(vm, vm, vm),
        scratch_shapes=[
            pltpu.VMEM((rows, width), BF16),
            pltpu.VMEM((3, rows, chan), BF16),
            pltpu.VMEM((rows, chan), F32),
            pltpu.VMEM((width // 128, 128), BF16),
            pltpu.VMEM((4, chan), BF16),
            pltpu.VMEM(rate_weight.shape, BF16),
            pltpu.VMEM(input_weight.shape, BF16),
            pltpu.VMEM((1, chan), F32),
            pltpu.VMEM((width // 128, 128), BF16),
            pltpu.VMEM((topk, rows), jnp.int32),
            pltpu.VMEM((topk, rows), F32),
            pltpu.VMEM((chan, width), BF16),
            pltpu.VMEM((width, 2 * ff), BF16),
            pltpu.VMEM((ff, width), BF16),
            pltpu.VMEM((2 * nz, rows, kh), BF16),
            pltpu.VMEM((2, nz * rows, kh), BF16),
            pltpu.VMEM((2, NX * ks, chan), BF16),
            pltpu.VMEM((2, nz * rows, chan), F32),
            pltpu.VMEM((4, half_z, rows, chan), BF16),
            pltpu.VMEM((4, half_z, rows, chan), BF16),
            pltpu.VMEM((NY, rows, chan), BF16),
            pltpu.VMEM((NY, rows, chan), BF16),
            pltpu.VMEM((NY, rows, chan), BF16),
            pltpu.VMEM((NY, rows, chan), BF16),
            pltpu.VMEM((2 * slots, ch), BF16),
            pltpu.VMEM((tp_n, 2 * slots, ch), BF16),
            pltpu.VMEM((width // 128, 128), F32),
            pltpu.VMEM((2, hs, 2 * ff), F32),
            pltpu.VMEM((2, NY, hs, chan), BF16),
            pltpu.VMEM((2, NY, hs, chan), BF16),
            pltpu.VMEM((2, 4, hs // 2, chan), F32),
            pltpu.VMEM((2, 6, hs // 2, chan), BF16),
            pltpu.VMEM((2, 2, hs // 2, chan), BF16),
            pltpu.VMEM((2, 2, 2, hs // 2, chan), BF16),
            pltpu.VMEM((2 * slots, ch), BF16),
            pltpu.VMEM((2 * slots, ch), BF16),
            dma((17,)),
            dma((2,)),
            dma((2, NX, 2)),
            dma((1,)),
            dma((nz,)),
            dma((1,)),
            dma((1,)),
            dma((4,)),
            dma((4, half_z)),
            dma((1,)),
            dma((NY,)),
            dma((1,)),
            dma((NY,)),
            dma((1,)),
            dma((2,)),
            dma((2,)),
            dma((NY, 2, 2)),
            dma((NY, 2)),
            dma((2,)),
            dma((2, NY)),
            dma((2,)),
            dma((2, 2)),
            dma((2, 2)),
            dma((1,)),
            dma((2,)),
        ],
        compiler_params=pltpu.CompilerParams(
            collective_id=0,
            has_side_effects=True,
            vmem_limit_bytes=66000000,
        ),
        name="layer",
    )(
        tokens,
        conv_in.transpose(1, 0, 2),
        state_in,
        mix_gain.reshape(width // 128, 128),
        rnn_weight,
        gate_weight,
        conv_weight,
        rate_weight,
        input_weight,
        rate_param.reshape(1, chan),
        moe_gain.reshape(width // 128, 128),
        routes.T,
        route_prob.T,
        out_weight,
        expert_gate,
        expert_up,
        expert_down,
    )
    layer_out, state_out, conv_out = pl.pallas_call(
        finish_kernel,
        out_shape=shapes,
        in_specs=[vm] * 3,
        out_specs=(hbm, hbm, hbm),
        scratch_shapes=[dma((3,))],
        compiler_params=pltpu.CompilerParams(vmem_limit_bytes=4 * 1024 * 1024),
        name="finish",
    )(*outs)
    return (layer_out, state_out, conv_out.transpose(1, 0, 2))


def solution(mesh):
    in_specs = (
        P("ep", None),
        P("ep", "tp"),
        P("ep", None, "tp"),
        P(),
        P("ep", "tp"),
        P("ep", "tp"),
        P(None, "tp"),
        P("tp", None, None),
        P("tp", None, None),
        P("tp"),
        P("tp", None),
        P(),
        P("ep", None, "tp"),
        P("ep", None, "tp"),
        P("ep", "tp", None),
        P("ep", None),
        P("ep", None),
    )
    out_specs = (P("ep", "tp"), P("ep", "tp"), P("ep", None, "tp"))
    return jax.shard_map(shards, mesh=mesh, in_specs=in_specs, out_specs=out_specs, check_vma=False)
```
